32 devices in a mesh: sp: 8 (over z, x), tp: 4 (over y, core).
Axes of the slice: x: 2, y: 2, z: 4, core: 2. Of those that a mesh axis runs over, the one named last changes fastest.
Arguments:
- inputs: bfloat16 [3072, 2048], P('sp', 'tp'), may hold values from -6 to 6
- norm_gain: float32 [2048], replicated, may hold values from 0.1 to 1.9
- query_weight: bfloat16 [2048, 1024], P(None, 'tp')
- key_weight: bfloat16 [2048, 1024], P(None, 'tp'), may hold values from -0.15625 to 0.15625
- value_weight: bfloat16 [2048, 1024], P(None, 'tp'), may hold values from -0.125 to 0.125
- memory_query_weight: bfloat16 [2048, 1024], P(None, 'tp'), may hold values from -0.125 to 0.125
- memory_key_weight: bfloat16 [2048, 1024], P(None, 'tp'), may hold values from -0.125 to 0.125
- memory_value_weight: bfloat16 [2048, 1024], P(None, 'tp'), may hold values from -0.125 to 0.125
- input_gate_weight: bfloat16 [2048, 16], P(None, 'tp')
- forget_gate_weight: bfloat16 [2048, 16], P(None, 'tp'), may hold values from -0.3125 to 0.3125
- forget_bias: float32 [16], P('tp'), may hold values from 3 to 13
- decay_shift: float32 [3072, 16], P('sp', 'tp'), may hold values from -2 to 0, as said below
- lambdas: float32 [16], P('tp'), may hold values from 0.3 to 0.8
- head_gain: float32 [64], replicated, may hold values from 0.1 to 1.9
- out_weight_attention: bfloat16 [1024, 2048], P('tp'), may hold values from -0.125 to 0.125
- out_weight_memory: bfloat16 [1024, 2048], P('tp'), may hold values from -0.125 to 0.125
Outputs:
- combined: bfloat16 [3072, 2048], P('sp', 'tp')
The draws below stay inside these ranges and needn't reach their ends.
Inputs may be any that keep to these rules, and one draw needn't show every extreme that they name: `decay_shift`: never positive.
All inputs are finite; a program needn't handle non-finite values.
Results may differ from the reference program's by a relative error of at most 0.018.
The reference program's roundings to bfloat16 on the way count: a program that leaves them out, or rounds other values in their place, can miss the bound.
Values may be sent and summed in bfloat16 or wider, within the bound.
A program may use at most 192 MiB of HBM per device.

```python
import math
import jax
import jax.numpy as jnp
from jax import lax

D = 2048
HEAD = 64
DD = 32
HD = 16
MATRIX_HEADS = 16
BLOCK = 64
SEQUENCE_TOKENS = 3072
N_TP = 4


def draw_query_weight(key, part):
    entries = jnp.clip(jax.random.normal(jax.random.fold_in(key, 11), (D, HD * HEAD), jnp.float32), -6.0, 6.0)
    entries = entries * (1.3 / D ** 0.5)
    return entries.astype(jnp.bfloat16)


def draw_input_gate_weight(key, part):
    entries = jnp.clip(jax.random.normal(jax.random.fold_in(key, 13), (D, MATRIX_HEADS), jnp.float32), -6.0, 6.0)
    entries = entries / D ** 0.5
    return entries.astype(jnp.bfloat16)


def draw_forget_bias(key, part):
    fast_share = 0.5
    fast_heads = jax.random.uniform(jax.random.fold_in(key, 21), (MATRIX_HEADS,), jnp.float32) < fast_share
    jitter = jax.random.uniform(jax.random.fold_in(key, 22), (MATRIX_HEADS,), jnp.float32)
    quick_bias = math.log(40.0) + jitter - 0.5
    slow_bias = math.log(float(SEQUENCE_TOKENS)) + 2.0 + jitter
    return jnp.where(fast_heads, quick_bias, slow_bias).astype(jnp.float32)


def draw_decay_shift(key, part):
    block_count = SEQUENCE_TOKENS // BLOCK
    factor = jnp.exp(jax.random.uniform(jax.random.fold_in(key, 31), (block_count, 1, MATRIX_HEADS), jnp.float32, math.log(0.3), math.log(5.0)))
    constant_level = -jnp.broadcast_to(factor, (block_count, BLOCK, MATRIX_HEADS)).reshape(SEQUENCE_TOKENS, MATRIX_HEADS) / SEQUENCE_TOKENS
    spike_row_list = jax.random.randint(jax.random.fold_in(key, 32), (4, MATRIX_HEADS), 0, SEQUENCE_TOKENS)
    spike_dropouts = jnp.log(jax.random.uniform(jax.random.fold_in(key, 33), (4, MATRIX_HEADS), jnp.float32, 0.4, 0.75))
    row_indices = jnp.arange(SEQUENCE_TOKENS, dtype=jnp.int32)[:, None, None]
    spike_events = jnp.sum(jnp.where(row_indices == spike_row_list[None], spike_dropouts[None], 0.0), axis=1)
    return jnp.maximum(constant_level + spike_events, -2.0).astype(jnp.float32)


def levels(own_key, extent, cuts, low, top_value):
    def one(position, parts):
        draws = jax.random.uniform(jax.random.fold_in(jax.random.fold_in(own_key, 6), position), (parts,), jnp.float32, low / len(cuts), top_value / len(cuts))
        return jnp.repeat(jnp.exp(draws), extent[position] // parts).reshape((-1,) + (1,) * (len(extent) - position - 1))

    gain = one(*cuts[0])
    for cut in cuts[1:]:
        gain = gain * one(*cut)
    return gain


def centred(own_key, extent, deviation, bound, shards=(), kind=jnp.bfloat16):
    drawn = deviation * jax.random.normal(own_key, extent, jnp.float32)
    if shards:
        drawn = drawn * levels(own_key, extent, shards, -0.22, 0.18)
    return jnp.clip(drawn, -bound, bound).astype(kind)


def setup_inputs(seed: int = 0) -> dict:
    key_of = jax.random.split(jax.random.key(seed), 17)
    return {
        "inputs": centred(key_of[0], (SEQUENCE_TOKENS, D), 1.0, 6.0, ((0, 8), (1, 4))),
        "norm_gain": jnp.clip(1.0 + 0.18 * jax.random.normal(key_of[1], (D,), jnp.float32), 0.1, 1.9),
        "query_weight": draw_query_weight(jax.random.fold_in(key_of[16], 71), 0),
        "key_weight": centred(key_of[3], (D, HD * HEAD), (D * 10 // 17) ** -0.5, 0.15625, ((1, 4),)),
        "value_weight": centred(key_of[4], (D, HD * HEAD), D ** -0.5, 0.125, ((1, 4),)),
        "memory_query_weight": centred(key_of[5], (D, MATRIX_HEADS * HEAD), D ** -0.5, 0.125, ((1, 4),)),
        "memory_key_weight": centred(key_of[6], (D, MATRIX_HEADS * HEAD), D ** -0.5, 0.125, ((1, 4),)),
        "memory_value_weight": centred(key_of[7], (D, MATRIX_HEADS * HEAD), D ** -0.5, 0.125, ((1, 4),)),
        "input_gate_weight": draw_input_gate_weight(jax.random.fold_in(key_of[16], 71), 0),
        "forget_gate_weight": centred(key_of[9], (D, MATRIX_HEADS), (D // 6) ** -0.5, 0.3125, ((1, 4),)),
        "forget_bias": draw_forget_bias(jax.random.fold_in(key_of[16], 71), 0),
        "decay_shift": draw_decay_shift(jax.random.fold_in(key_of[16], 71), 0),
        "lambdas": jnp.clip(0.3 + 0.5 * jax.random.uniform(key_of[12], (HD,), jnp.float32) ** levels(key_of[12], (HD,), ((0, 4),), -0.2, 0.2), 0.3, 0.8),
        "head_gain": jnp.clip(1.0 + 0.18 * jax.random.normal(key_of[13], (HEAD,), jnp.float32), 0.1, 1.9),
        "out_weight_attention": centred(key_of[14], (HD * HEAD, D), ((HD + MATRIX_HEADS) * HEAD) ** -0.5, 0.125, ((0, 4),)),
        "out_weight_memory": centred(key_of[15], (MATRIX_HEADS * HEAD, D), ((HD + MATRIX_HEADS) * HEAD) ** -0.5, 0.125, ((0, 4),)),
    }


EPSILON = 1e-06
ROTARY_BASE = 10000.0
NEGATIVE = -1e+30

def rotate(halves, positions):
    middle = halves.shape[-1] // 2
    inverse = 1.0 / ROTARY_BASE ** (jnp.arange(middle, dtype=jnp.float32) / middle)
    angles = positions.astype(jnp.float32)[:, None] * inverse[None, :]
    cosine = jnp.cos(angles)[:, None, :]
    sine_part = jnp.sin(angles)[:, None, :]
    floats = halves.astype(jnp.float32)
    former = floats[..., :middle]
    latter = floats[..., middle:]
    turned = jnp.concatenate([former * cosine - latter * sine_part, latter * cosine + former * sine_part], axis=-1)
    return turned.astype(jnp.bfloat16)

def advance_state(carried, block_entry):
    memory, normal, stable = carried
    block_memory, block_normal, block_max, block_decay = block_entry
    new_stable = jnp.maximum(block_decay + stable, block_max)
    former = jnp.exp(block_decay + stable - new_stable)
    latter = jnp.exp(block_max - new_stable)
    return (former[:, None, None] * memory + latter[:, None, None] * block_memory, former[:, None] * normal + latter[:, None] * block_normal, new_stable)

def memory_blocks(queries, key_heads, values, gate_in, log_forget, entering):
    token_count, head_count, head_width = queries.shape
    block_count = token_count // BLOCK
    highest = lax.Precision.HIGHEST

    def blocked(flat_array):
        return flat_array.astype(jnp.float32).reshape(block_count, BLOCK, head_count, head_width).transpose(2, 0, 1, 3)
    query_blocks = blocked(queries)
    key_blocks = blocked(key_heads) * head_width ** (-0.5)
    value_blocks = blocked(values)
    gate_blocks = gate_in.reshape(block_count, BLOCK, head_count).transpose(2, 0, 1)
    cumulative = jnp.cumsum(log_forget.reshape(block_count, BLOCK, head_count).transpose(2, 0, 1), axis=-1)
    block_ends = cumulative[..., -1]
    toward_end = block_ends[..., None] - cumulative + gate_blocks
    local_max = lax.optimization_barrier(jnp.max(toward_end, axis=-1))
    end_weights = jnp.exp(toward_end - local_max[..., None])
    local_memory = jnp.einsum('hcl,hclv,hclk->chvk', end_weights, value_blocks, key_blocks, precision=highest)
    local_normal = jnp.einsum('hcl,hclk->chk', end_weights, key_blocks, precision=highest)

    def scan_step(carried, block_entry):
        return (advance_state(carried, block_entry), carried)
    entries = (local_memory, local_normal, local_max.T, block_ends.T)
    unused, (memory_in, normal_in, stable_in) = lax.scan(scan_step, entering, entries)
    lower_mask = jnp.tril(jnp.ones((BLOCK, BLOCK), dtype=bool))
    decays = jnp.where(lower_mask, cumulative[..., :, None] - cumulative[..., None, :] + gate_blocks[..., None, :], NEGATIVE)
    carried_log = cumulative + stable_in.T[..., None]
    row_max = jnp.maximum(carried_log, lax.optimization_barrier(jnp.max(decays, axis=-1)))
    within = jnp.where(lower_mask, jnp.exp(decays - row_max[..., None]), 0.0)
    outside = jnp.exp(carried_log - row_max)
    scores = within * jnp.einsum('hctd,hcsd->hcts', query_blocks, key_blocks, precision=highest)
    numerator = outside[..., None] * jnp.einsum('chvk,hctk->hctv', memory_in, query_blocks, precision=highest)
    numerator = numerator + jnp.einsum('hcts,hcsv->hctv', scores, value_blocks, precision=highest)
    denominator = outside * jnp.einsum('chk,hctk->hct', normal_in, query_blocks, precision=highest) + lax.optimization_barrier(jnp.sum(scores, axis=-1))
    result = numerator / jnp.maximum(jnp.abs(denominator), 1.0)[..., None]
    return result.transpose(1, 2, 0, 3).reshape(token_count, head_count * head_width).astype(jnp.bfloat16)

def differential(query_first, query_second, key_first, key_second, values, lambdas, head_gain):
    token_count = query_first.shape[0]
    query_span = min(512, token_count)
    score_scale = DD ** (-0.5)
    key_positions = jnp.arange(token_count, dtype=jnp.int32)

    def per_head(head_entry):
        head_query_first, head_query_second, head_key_first, head_key_second, value_head, factor = head_entry

        def per_block(block_index):
            first_row = block_index * query_span
            query_positions = first_row + jnp.arange(query_span, dtype=jnp.int32)
            visible = key_positions[None, :] <= query_positions[:, None]
            results = []
            for query_side, key_side in ((head_query_first, head_key_first), (head_query_second, head_key_second)):
                query_block = lax.dynamic_slice_in_dim(query_side, first_row, query_span, 0)
                scores = jnp.dot(query_block, key_side.T, preferred_element_type=jnp.float32) * score_scale
                scores = jnp.where(visible, scores, NEGATIVE)
                row_max = lax.optimization_barrier(jnp.max(scores, axis=1, keepdims=True))
                weights = jnp.where(visible, jnp.exp(scores - row_max), 0.0)
                totals = lax.optimization_barrier(jnp.sum(weights, axis=1, keepdims=True))
                results.append(jnp.dot(weights.astype(jnp.bfloat16), value_head, preferred_element_type=jnp.float32) / totals)
            return results[0] - factor * results[1]
        return lax.map(per_block, jnp.arange(token_count // query_span, dtype=jnp.int32))
    entries = (query_first.transpose(1, 0, 2), query_second.transpose(1, 0, 2), key_first.transpose(1, 0, 2), key_second.transpose(1, 0, 2), values.transpose(1, 0, 2), lambdas)
    stacked = lax.map(per_head, entries)
    head_count = stacked.shape[0]
    stacked = stacked.reshape(head_count, token_count, -1).transpose(1, 0, 2)
    norm_scale = lax.rsqrt(lax.optimization_barrier(jnp.mean(stacked * stacked, axis=-1, keepdims=True)) + EPSILON)
    return (stacked * norm_scale * head_gain).astype(jnp.bfloat16).reshape(token_count, -1)

def reference(inputs, norm_gain, query_weight, key_weight, value_weight, memory_query_weight, memory_key_weight, memory_value_weight, input_gate_weight, forget_gate_weight, forget_bias, decay_shift, lambdas, head_gain, out_weight_attention, out_weight_memory):
    token_count = inputs.shape[0]
    floats = inputs.astype(jnp.float32)
    inverse_rms = lax.rsqrt(lax.optimization_barrier(jnp.mean(floats * floats, axis=1, keepdims=True)) + EPSILON)
    scaled = (floats * norm_gain[None, :]).astype(jnp.bfloat16)

    def project(weight):
        return jnp.dot(scaled, weight, preferred_element_type=jnp.float32) * inverse_rms

    def split_heads(weight):
        return project(weight).astype(jnp.bfloat16).reshape(token_count, -1, HEAD)
    positions = jnp.arange(token_count, dtype=jnp.int32)
    queries = split_heads(query_weight)
    key_heads = split_heads(key_weight)
    values = split_heads(value_weight)
    attended = differential(rotate(queries[..., :DD], positions), rotate(queries[..., DD:], positions), rotate(key_heads[..., :DD], positions), rotate(key_heads[..., DD:], positions), values, lambdas, head_gain)
    gate_in = project(input_gate_weight)
    log_forget = jax.nn.log_sigmoid(project(forget_gate_weight) + forget_bias[None, :]) + decay_shift
    head_count = gate_in.shape[1]
    entering = (jnp.zeros((head_count, HEAD, HEAD), jnp.float32), jnp.zeros((head_count, HEAD), jnp.float32), jnp.zeros((head_count,), jnp.float32))
    memory = memory_blocks(split_heads(memory_query_weight), split_heads(memory_key_weight), split_heads(memory_value_weight), gate_in, log_forget, entering)
    attended_width = attended.shape[1] // N_TP
    memory_width = memory.shape[1] // N_TP
    combined = jnp.zeros((token_count, out_weight_attention.shape[1]), jnp.float32)
    for group_index in range(N_TP):
        low_a = group_index * attended_width
        low_m = group_index * memory_width
        partial_sum = jnp.dot(attended[:, low_a:low_a + attended_width], out_weight_attention[low_a:low_a + attended_width], preferred_element_type=jnp.float32)
        partial_sum = partial_sum + jnp.dot(memory[:, low_m:low_m + memory_width], out_weight_memory[low_m:low_m + memory_width], preferred_element_type=jnp.float32)
        combined = combined + lax.optimization_barrier(partial_sum.astype(jnp.bfloat16)).astype(jnp.float32)
    return combined.astype(jnp.bfloat16)
```

```python
import functools

import jax
import jax.numpy as jnp
from jax import lax
from jax.experimental import pallas as pl
from jax.experimental.pallas import tpu as pltpu
from jax.sharding import PartitionSpec as P

HEAD = 64
DD = 32
EPSILON = 1e-06
ROTARY_BASE = 10000.0
NEGATIVE = -1e30
LOG2E = 1.4426950408889634
CORES = 2
STATE_ROWS = HEAD + 8
VMEM = pl.BlockSpec(memory_space=pltpu.VMEM)
MESH = pl.DeviceIdType.MESH
VMEM_LIMIT = 60 * 1024 * 1024


def signal(semaphore, axis, place):
    pl.semaphore_signal(semaphore, inc=1, device_id={axis: place}, device_id_type=MESH)


def remote(source, target, send_sem, recv_sem, axis, place):
    return pltpu.make_async_remote_copy(
        src_ref=source,
        dst_ref=target,
        send_sem=send_sem,
        recv_sem=recv_sem,
        device_id={axis: place},
        device_id_type=MESH,
    )


def tp_barrier(me, row_places):
    core = lax.rem(me, CORES)
    line = me // CORES
    barrier = pltpu.get_barrier_semaphore()
    signal(barrier, "tp", line * CORES + (1 - core))
    for step in range(1, row_places):
        signal(barrier, "tp", lax.rem(line + step, row_places) * CORES + core)
    pl.semaphore_wait(barrier, row_places)


def gather_kernel(size, chunks, x_ref, out_ref, local_sem, send_sems, recv_sems, pair_send, pair_recv):
    rows, columns = x_ref.shape
    lines = size // CORES
    me = lax.axis_index("tp")
    core = lax.rem(me, CORES)
    line = me // CORES
    pair = line * CORES + (1 - core)
    tp_barrier(me, lines)
    span = rows // chunks

    def place(owner, chunk):
        return out_ref.at[
            pl.ds(chunk * span, span), pl.ds(pl.multiple_of(owner * columns, 128), columns)
        ]

    sends = []
    for chunk in range(chunks):
        for step in range(1, lines):
            other = lax.rem(line + step, lines) * CORES + core
            copy = remote(
                x_ref.at[pl.ds(chunk * span, span)],
                place(me, chunk),
                send_sems.at[step, chunk],
                recv_sems.at[step, chunk],
                "tp",
                other,
            )
            copy.start()
            sends.append(copy)
    own = pltpu.make_async_copy(
        x_ref, out_ref.at[:, pl.ds(pl.multiple_of(me * columns, 128), columns)], local_sem
    )
    own.start()
    pairs = []
    for chunk in range(chunks):
        copy = remote(
            x_ref.at[pl.ds(chunk * span, span)],
            place(me, chunk),
            pair_send.at[0, chunk],
            pair_recv.at[0, chunk],
            "tp",
            pair,
        )
        copy.start()
        pairs.append(copy)
    for chunk in range(chunks):
        for step in range(1, lines):
            source = lax.rem(line + lines - step, lines) * CORES + core
            arrived = remote(
                place(source, chunk),
                place(source, chunk),
                send_sems.at[step, chunk],
                recv_sems.at[step, chunk],
                "tp",
                pair,
            )
            arrived.wait_recv()
            copy = remote(
                place(source, chunk),
                place(source, chunk),
                pair_send.at[step, chunk],
                pair_recv.at[step, chunk],
                "tp",
                pair,
            )
            copy.start()
            pairs.append(copy)
    own.wait()
    for copy in sends:
        copy.wait_send()
    for copy in pairs:
        copy.wait()


def head_mask(width, head):
    lanes = lax.broadcasted_iota(jnp.int32, (1, width), 1)
    return (lanes // HEAD) == head


def spread(columns, width):
    spreaded = columns[:, 0:1]
    for head in range(1, columns.shape[1]):
        lanes = lax.broadcasted_iota(jnp.int32, (1, width), 1)
        spreaded = jnp.where(lanes >= head * HEAD, columns[:, head : head + 1], spreaded)
    return jnp.broadcast_to(spreaded, (columns.shape[0], width))


def two_parts(floats):
    high = floats.astype(jnp.bfloat16)
    return high, (floats - high.astype(jnp.float32)).astype(jnp.bfloat16)


def dot(a, b, dims=((1,), (0,))):
    return lax.dot_general(a, b, (dims, ((), ())), preferred_element_type=jnp.float32)


def project_kernel(
    x_ref, gain_ref, cos_ref, sin_ref, wq, wk, wv, wmq, wmk, wmv, wi, wf, bias_ref, shift_ref,
    q_out, kv_out, mq_out, mk_out, mv_out, gate_out, gate_row_out, state_out,
    sq, sk, sv, smq, smk, smv, sems,
):
    copies = []
    for place, (source, target) in enumerate(
        ((wq, sq), (wk, sk), (wv, sv), (wmq, smq), (wmk, smk), (wmv, smv))
    ):
        copy = pltpu.make_async_copy(source, target, sems.at[place])
        copy.start()
        copies.append(copy)
    rows, features = x_ref.shape
    width = q_out.shape[1]
    heads = width // HEAD
    floats = x_ref[...].astype(jnp.float32)
    inverse = lax.rsqrt(
        jnp.sum(floats * floats, axis=1, keepdims=True) / features + EPSILON
    )
    scaled = (floats * gain_ref[...]).astype(jnp.bfloat16)
    gate = dot(scaled, wi[...]) * inverse
    pre = dot(scaled, wf[...]) * inverse + bias_ref[...]
    forget = jnp.minimum(pre, 0.0) - jnp.log1p(jnp.exp(-jnp.abs(pre))) + shift_ref[...]
    row_index = lax.broadcasted_iota(jnp.int32, (rows, rows), 0)
    column_index = lax.broadcasted_iota(jnp.int32, (rows, rows), 1)
    lower = (column_index <= row_index).astype(jnp.bfloat16)
    first, rest = two_parts(forget)
    second = (forget - first.astype(jnp.float32) - rest.astype(jnp.float32)).astype(jnp.bfloat16)
    cumulative = dot(lower, first) + (dot(lower, rest) + dot(lower, second))

    def product(place, scratch):
        copies[place].wait()
        return (dot(scaled, scratch[...]) * inverse).astype(jnp.bfloat16)

    lanes = lax.broadcasted_iota(jnp.int32, (1, width), 1)
    former = lax.rem(lanes, DD) < DD // 2

    def rotated(values):
        wide = values.astype(jnp.float32)
        partner = jnp.where(
            former, pltpu.roll(wide, width - DD // 2, 1), pltpu.roll(wide, DD // 2, 1)
        )
        return (wide * cos_ref[...] + partner * sin_ref[...]).astype(jnp.bfloat16)

    q_out[...] = rotated(product(0, sq))
    kv_out[:, :width] = rotated(product(1, sk))
    kv_out[:, width:] = product(2, sv)
    mq_out[...] = product(3, smq)
    memory_keys = product(4, smk)
    memory_values = product(5, smv)
    mk_out[...] = memory_keys
    mv_out[...] = memory_values

    end = cumulative[rows - 1 : rows, :]
    toward = end - cumulative + gate
    top = jnp.max(toward, axis=0, keepdims=True)
    weights = spread(jnp.exp(toward - top), width)
    keyed = memory_keys.astype(jnp.float32) * (HEAD**-0.5) * weights
    high, low = two_parts(keyed)
    whole = dot(high, memory_values, ((0,), (0,))) + dot(low, memory_values, ((0,), (0,)))
    memory = jnp.zeros((HEAD, width), jnp.float32)
    for head in range(heads):
        memory = jnp.where(
            head_mask(width, head), whole[head * HEAD : (head + 1) * HEAD, :], memory
        )
    state_out[:HEAD, :] = memory
    state_out[HEAD : HEAD + 1, :] = jnp.sum(keyed, axis=0, keepdims=True)
    state_out[HEAD + 1 : HEAD + 2, :] = spread(top, width)
    state_out[HEAD + 2 : HEAD + 3, :] = spread(end, width)
    state_out[HEAD + 3 :, :] = jnp.zeros((STATE_ROWS - HEAD - 3, width), jnp.float32)
    gate_out[...] = cumulative
    offsets = jnp.concatenate(
        [gate - cumulative, jnp.zeros((rows, 128 - heads), jnp.float32)], axis=1
    )
    gate_row_out[...] = offsets.T[:8, :]


def exchange_kernel(depth, across, kv_ref, state_ref, kv_all, state_all, local_sems, kv_send, kv_recv, st_send, st_recv):
    me = lax.axis_index("sp")
    z = me // across
    x = lax.rem(me, across)
    barrier = pltpu.get_barrier_semaphore()

    @pl.when(z > 0)
    def _():
        signal(barrier, "sp", me - across)

    @pl.when(z < depth - 1)
    def _():
        signal(barrier, "sp", me + across)

    for step in range(1, across):
        signal(barrier, "sp", z * across + lax.rem(x + step, across))
    beside = (z > 0).astype(jnp.int32) + (z < depth - 1).astype(jnp.int32)
    pl.semaphore_wait(barrier, across - 1 + beside)

    own_kv = pltpu.make_async_copy(kv_ref, kv_all.at[me], local_sems.at[0])
    own_state = pltpu.make_async_copy(state_ref, state_all.at[me], local_sems.at[1])
    own_kv.start()
    own_state.start()

    def transfers(back, slot, target, place):
        for source, everything, send, recv in (
            (state_ref, state_all, st_send, st_recv),
            (kv_ref, kv_all, kv_send, kv_recv),
        ):
            yield remote(
                source if back == 0 else everything.at[slot],
                everything.at[slot],
                send.at[back, target],
                recv.at[slot],
                "sp",
                place,
            )

    def rounds(act):
        for back in range(depth):
            slot = me - back * across

            def moves():
                @pl.when(z < depth - 1)
                def _():
                    for copy in transfers(back, slot, 0, me + across):
                        act(copy)

                for step in range(1, across):
                    other = lax.rem(x + step, across)
                    needed = (x < other) if back == 0 else (z >= back)

                    @pl.when(needed)
                    def _():
                        for copy in transfers(back, slot, step, z * across + other):
                            act(copy)

            yield back, slot, moves

    for back, slot, moves in rounds(lambda copy: copy.start()):
        if back == 0:
            moves()
        else:

            @pl.when(z >= back)
            def _():
                for copy in transfers(back, slot, 0, me):
                    copy.wait_recv()
                moves()

    for back in range(depth):
        for step in range(1, across):
            other = lax.rem(x + step, across)
            slot = (z - back) * across + other
            arriving = (other < x) if back == 0 else (z >= back)

            @pl.when(arriving)
            def _():
                for copy in transfers(1, slot, 0, me):
                    copy.wait_recv()

    for back, slot, moves in rounds(lambda copy: copy.wait_send()):
        if back == 0:
            moves()
        else:
            pl.when(z >= back)(moves)
    own_kv.wait()
    own_state.wait()


def mixer_kernel(
    q_ref, kv_ref, mq_ref, mk_ref, mv_ref, cumulative_ref, offset_ref, state_ref,
    lambda_ref, gain_ref, woa, wom, out_ref, attended_ref, memory_ref, soa, som,
    chosen_ref, top_ref, total_ref, sums_ref, sems,
):
    load_attention = pltpu.make_async_copy(woa, soa, sems.at[0])
    load_memory = pltpu.make_async_copy(wom, som, sems.at[1])
    load_attention.start()
    load_memory.start()
    me = lax.axis_index("sp")
    rows, width = q_ref.shape
    heads = width // HEAD
    row_index = lax.broadcasted_iota(jnp.int32, (rows, rows), 0)
    column_index = lax.broadcasted_iota(jnp.int32, (rows, rows), 1)
    lower = column_index <= row_index
    factor = (DD**-0.5) * LOG2E
    lanes = lax.broadcasted_iota(jnp.int32, (1, 128), 1)

    state = jnp.zeros((STATE_ROWS, width), jnp.float32)

    def advance(place, carried):
        body, stable = carried
        later = state_ref[place]
        later_top = later[HEAD + 1 : HEAD + 2, :]
        decay = later[HEAD + 2 : HEAD + 3, :]
        new = jnp.maximum(decay + stable, later_top)
        return jnp.exp(decay + stable - new) * body + jnp.exp(later_top - new) * later, new

    state, stable = lax.fori_loop(0, me, advance, (state, jnp.zeros((1, width), jnp.float32)))
    memory_in = state[:HEAD, :]
    normal_in = state[HEAD : HEAD + 1, :]
    blocks = jnp.concatenate(
        [jnp.where(head_mask(width, head), memory_in, 0.0) for head in range(heads)], axis=0
    )
    high, low = two_parts(blocks)
    memory_queries = mq_ref[...]
    carried_part = dot(memory_queries, high) + dot(memory_queries, low)
    weighted = memory_queries.astype(jnp.float32) * normal_in
    for group in range(width // 128):
        span = slice(group * 128, (group + 1) * 128)
        keys = mk_ref[:, span]
        values = mv_ref[:, span]
        group_queries = mq_ref[:, span]
        result = None
        for side in range(2):
            head = group * 2 + side
            chosen = (lanes // HEAD) == side
            column = cumulative_ref[:, head : head + 1]
            gaps = jnp.where(lower, column + offset_ref[head : head + 1, :], NEGATIVE)
            carried_log = column + stable[:, head * HEAD : head * HEAD + 1]
            row_top = jnp.maximum(carried_log, jnp.max(gaps, axis=1, keepdims=True))
            within = jnp.exp(gaps - row_top)
            outside = jnp.exp(carried_log - row_top)
            scores = dot(jnp.where(chosen, group_queries, 0), keys, ((1,), (1,)))
            scores = jnp.where(lower, within * (scores * (HEAD**-0.5)), 0.0)
            denominator = jnp.sum(scores, axis=1, keepdims=True) + outside * jnp.sum(
                jnp.where(chosen, weighted[:, span], 0.0), axis=1, keepdims=True
            )
            score_high, score_low = two_parts(scores)
            numerator = dot(score_high, values) + dot(score_low, values)
            numerator = numerator + outside * carried_part[:, span]
            quotient = numerator / jnp.maximum(jnp.abs(denominator), 1.0)
            result = quotient if result is None else jnp.where(chosen, quotient, result)
        memory_ref[:, span] = result.astype(jnp.bfloat16)

    upper = row_index <= column_index
    for head in range(heads):
        group = slice(head // 2 * 128, head // 2 * 128 + 128)
        for half in range(2):
            chosen = (lanes // DD) == (head % 2) * 2 + half
            chosen_ref[head * 2 + half] = jnp.where(chosen, q_ref[:, group], 0)

    def block(place, diagonal):
        for head in range(heads):
            group = slice(head // 2 * 128, head // 2 * 128 + 128)
            value_group = slice(width + head // 2 * 128, width + head // 2 * 128 + 128)
            if head % 2 == 0:
                turned = kv_ref[place, :, value_group].T
            values = turned[(head % 2) * HEAD : (head % 2 + 1) * HEAD, :]
            for half in range(2):
                index = head * 2 + half
                at = slice(index, index + 1)
                rows_at = slice(index * HEAD, (index + 1) * HEAD)
                scores = dot(kv_ref[place, :, group], chosen_ref[index], ((1,), (1,)))
                if diagonal:
                    scores = jnp.where(upper, scores, NEGATIVE)
                top = jnp.max(scores, axis=0, keepdims=True)
                if not diagonal:
                    old_top = top_ref[at, :]
                    top = jnp.maximum(top, old_top)
                weights = jnp.exp2((scores - top) * factor)
                total = jnp.sum(weights, axis=0, keepdims=True)
                sums = dot(values, weights.astype(jnp.bfloat16))
                if not diagonal:
                    shrink = jnp.exp2((old_top - top) * factor)
                    total = total + total_ref[at, :] * shrink
                    sums = sums + sums_ref[rows_at, :] * shrink
                top_ref[at, :] = top
                total_ref[at, :] = total
                sums_ref[rows_at, :] = sums

    block(me, True)

    def earlier(place, unused):
        block(place, False)
        return unused

    lax.fori_loop(0, me, earlier, 0)
    for head in range(heads):
        first, second = (
            sums_ref[index * HEAD : (index + 1) * HEAD, :] / total_ref[index : index + 1, :]
            for index in (head * 2, head * 2 + 1)
        )
        difference = first - lambda_ref[:, head : head + 1] * second
        mean = jnp.mean(difference * difference, axis=0, keepdims=True)
        attended_ref[head * HEAD : (head + 1) * HEAD, :] = (
            difference * lax.rsqrt(mean + EPSILON) * gain_ref[...]
        ).astype(jnp.bfloat16)
    load_attention.wait()
    load_memory.wait()
    out_ref[...] = (
        dot(attended_ref[...], soa[...], ((0,), (0,))) + dot(memory_ref[...], som[...])
    ).astype(jnp.bfloat16)


def scatter_kernel(size, chunks, part_ref, out_ref, pair_in, line_out, line_in, pair_send, pair_recv, line_send, line_recv):
    rows, columns = out_ref.shape
    lines = size // CORES
    me = lax.axis_index("tp")
    core = lax.rem(me, CORES)
    line = me // CORES
    pair = line * CORES + (1 - core)
    tp_barrier(me, lines)
    span = rows // chunks

    def columns_of(owner):
        return pl.ds(pl.multiple_of(owner * columns, 128), columns)

    def rows_of(chunk):
        return pl.ds(chunk * span, span)

    order = list(range(1, lines)) + [0]
    pairs = {}
    for chunk in range(chunks):
        for step in order:
            target = lax.rem(line + step, lines) * CORES + (1 - core)
            copy = remote(
                part_ref.at[rows_of(chunk), columns_of(target)],
                pair_in.at[step, rows_of(chunk)],
                pair_send.at[step, chunk],
                pair_recv.at[step, chunk],
                "tp",
                pair,
            )
            copy.start()
            pairs[step, chunk] = copy

    def pair_sum(step, chunk):
        pairs[step, chunk].wait_recv()
        mine = part_ref[rows_of(chunk), columns_of(lax.rem(line + step, lines) * CORES + core)]
        return mine.astype(jnp.float32) + pair_in[step, rows_of(chunk), :].astype(jnp.float32)

    sends = {}
    for chunk in range(chunks):
        for step in range(1, lines):
            line_out[step, rows_of(chunk), :] = pair_sum(step, chunk).astype(jnp.bfloat16)
            copy = remote(
                line_out.at[step, rows_of(chunk)],
                line_in.at[step, rows_of(chunk)],
                line_send.at[step, chunk],
                line_recv.at[step, chunk],
                "tp",
                lax.rem(line + step, lines) * CORES + core,
            )
            copy.start()
            sends[step, chunk] = copy
    for chunk in range(chunks):
        total = pair_sum(0, chunk)
        for step in range(1, lines):
            sends[step, chunk].wait_recv()
            total = total + line_in[step, rows_of(chunk), :].astype(jnp.float32)
        out_ref[rows_of(chunk), :] = total.astype(jnp.bfloat16)
    for copy in pairs.values():
        copy.wait_send()
    for copy in sends.values():
        copy.wait_send()


def per_device(tp_size, depth, across, inputs, norm_gain, query_weight, key_weight, value_weight,
               memory_query_weight, memory_key_weight, memory_value_weight, input_gate_weight,
               forget_gate_weight, forget_bias, decay_shift, lambdas, head_gain,
               out_weight_attention, out_weight_memory):
    rows, columns = inputs.shape
    features = norm_gain.shape[0]
    width = query_weight.shape[1]
    heads = width // HEAD
    lines = tp_size // CORES
    spans = depth * across
    chunks = 4
    dma = pltpu.SemaphoreType.DMA

    def params(**more):
        return pltpu.CompilerParams(vmem_limit_bytes=VMEM_LIMIT, **more)

    gathered = pl.pallas_call(
        functools.partial(gather_kernel, tp_size, chunks),
        out_shape=jax.ShapeDtypeStruct((rows, features), jnp.bfloat16),
        in_specs=[VMEM],
        out_specs=VMEM,
        scratch_shapes=[dma(()), dma((lines, chunks)), dma((lines, chunks)), dma((lines, chunks)), dma((lines, chunks))],
        compiler_params=params(collective_id=0, has_side_effects=True),
        name="gather_inputs",
    )(inputs)

    middle = DD // 2
    inverse = 1.0 / ROTARY_BASE ** (jnp.arange(middle, dtype=jnp.float32) / middle)
    positions = lax.axis_index("sp") * rows + jnp.arange(rows, dtype=jnp.int32)
    angles = positions.astype(jnp.float32)[:, None] * inverse[None, :]
    cosine = jnp.cos(angles)
    sine = jnp.sin(angles)
    cosine = jnp.tile(cosine, (1, width // middle))
    sine = jnp.tile(jnp.concatenate([-sine, sine], axis=1), (1, width // DD))

    hbm = pl.BlockSpec(memory_space=pl.ANY)
    half = jax.ShapeDtypeStruct((rows, width), jnp.bfloat16)
    queries, packed, memory_queries, memory_keys, memory_values, cumulative, offsets, state = pl.pallas_call(
        project_kernel,
        out_shape=[
            half,
            jax.ShapeDtypeStruct((rows, 2 * width), jnp.bfloat16),
            half,
            half,
            half,
            jax.ShapeDtypeStruct((rows, heads), jnp.float32),
            jax.ShapeDtypeStruct((8, rows), jnp.float32),
            jax.ShapeDtypeStruct((STATE_ROWS, width), jnp.float32),
        ],
        in_specs=[VMEM] * 4 + [hbm] * 6 + [VMEM] * 4,
        out_specs=[VMEM] * 8,
        scratch_shapes=[pltpu.VMEM((features, width), jnp.bfloat16)] * 6 + [dma((6,))],
        compiler_params=params(),
        name="project",
    )(
        gathered, norm_gain[None, :], cosine, sine, query_weight, key_weight, value_weight,
        memory_query_weight, memory_key_weight, memory_value_weight, input_gate_weight,
        forget_gate_weight, forget_bias[None, :], decay_shift,
    )

    everything, states = pl.pallas_call(
        functools.partial(exchange_kernel, depth, across),
        out_shape=[
            jax.ShapeDtypeStruct((spans, rows, 2 * width), jnp.bfloat16),
            jax.ShapeDtypeStruct((spans, STATE_ROWS, width), jnp.float32),
        ],
        in_specs=[VMEM] * 2,
        out_specs=[VMEM] * 2,
        scratch_shapes=[dma((2,)), dma((depth, across)), dma((spans,)), dma((depth, across)), dma((spans,))],
        compiler_params=params(collective_id=1, has_side_effects=True),
        name="exchange_spans",
    )(packed, state)

    partial_term = pl.pallas_call(
        mixer_kernel,
        out_shape=jax.ShapeDtypeStruct((rows, features), jnp.bfloat16),
        in_specs=[VMEM] * 10 + [hbm] * 2,
        out_specs=VMEM,
        scratch_shapes=[
            pltpu.VMEM((width, rows), jnp.bfloat16),
            pltpu.VMEM((rows, width), jnp.bfloat16),
            pltpu.VMEM((width, features), jnp.bfloat16),
            pltpu.VMEM((width, features), jnp.bfloat16),
            pltpu.VMEM((2 * heads, rows, 128), jnp.bfloat16),
            pltpu.VMEM((2 * heads, rows), jnp.float32),
            pltpu.VMEM((2 * heads, rows), jnp.float32),
            pltpu.VMEM((2 * width, rows), jnp.float32),
            dma((2,)),
        ],
        compiler_params=params(),
        name="mixers",
    )(
        queries, everything, memory_queries, memory_keys, memory_values, cumulative, offsets,
        states, lambdas[None, :], head_gain[:, None], out_weight_attention,
        out_weight_memory,
    )

    return pl.pallas_call(
        functools.partial(scatter_kernel, tp_size, chunks),
        out_shape=jax.ShapeDtypeStruct((rows, columns), jnp.bfloat16),
        in_specs=[VMEM],
        out_specs=VMEM,
        scratch_shapes=[
            pltpu.VMEM((lines, rows, columns), jnp.bfloat16),
            pltpu.VMEM((lines, rows, columns), jnp.bfloat16),
            pltpu.VMEM((lines, rows, columns), jnp.bfloat16),
            dma((lines, chunks)), dma((lines, chunks)), dma((lines, chunks)), dma((lines, chunks)),
        ],
        compiler_params=params(collective_id=2, has_side_effects=True),
        name="scatter_output",
    )(partial_term)


def columns_across(mesh):
    spans = mesh.shape["sp"]
    try:
        places = {device.coords[0] for device in mesh.devices.flat}
        across = len(places)
    except AttributeError:
        across = 2
    return across if spans % across == 0 else 1


def solution(mesh):
    across = columns_across(mesh)
    in_specs = (
        P("sp", "tp"),
        P(),
        P(None, "tp"),
        P(None, "tp"),
        P(None, "tp"),
        P(None, "tp"),
        P(None, "tp"),
        P(None, "tp"),
        P(None, "tp"),
        P(None, "tp"),
        P("tp"),
        P("sp", "tp"),
        P("tp"),
        P(),
        P("tp", None),
        P("tp", None),
    )
    return jax.shard_map(
        functools.partial(
            per_device, mesh.shape["tp"], mesh.shape["sp"] // across, across
        ),
        mesh=mesh,
        in_specs=in_specs,
        out_specs=P("sp", "tp"),
        check_vma=False,
    )
```

```python
import functools

import jax
import jax.numpy as jnp
from jax import lax
from jax.experimental import pallas as pl
from jax.experimental.pallas import tpu as pltpu
from jax.sharding import PartitionSpec as P

HEAD = 64
DD = 32
EPSILON = 1e-06
ROTARY_BASE = 10000.0
NEGATIVE = -1e30
LOG2E = 1.4426950408889634
CORES = 2
STATE_ROWS = HEAD + 8
VMEM = pl.BlockSpec(memory_space=pltpu.VMEM)
MESH = pl.DeviceIdType.MESH
VMEM_LIMIT = 60 * 1024 * 1024


def signal(semaphore, axis, place):
    pl.semaphore_signal(semaphore, inc=1, device_id={axis: place}, device_id_type=MESH)


def remote(source, target, send_sem, recv_sem, axis, place):
    return pltpu.make_async_remote_copy(
        src_ref=source,
        dst_ref=target,
        send_sem=send_sem,
        recv_sem=recv_sem,
        device_id={axis: place},
        device_id_type=MESH,
    )


def tp_barrier(me, row_places):
    core = lax.rem(me, CORES)
    line = me // CORES
    barrier = pltpu.get_barrier_semaphore()
    signal(barrier, "tp", line * CORES + (1 - core))
    for step in range(1, row_places):
        signal(barrier, "tp", lax.rem(line + step, row_places) * CORES + core)
    pl.semaphore_wait(barrier, row_places)


def gather_kernel(size, chunks, x_ref, out_ref, local_sem, send_sems, recv_sems, pair_send, pair_recv):
    rows, columns = x_ref.shape
    lines = size // CORES
    me = lax.axis_index("tp")
    core = lax.rem(me, CORES)
    line = me // CORES
    pair = line * CORES + (1 - core)
    tp_barrier(me, lines)
    span = rows // chunks

    def place(owner, chunk):
        return out_ref.at[
            pl.ds(chunk * span, span), pl.ds(pl.multiple_of(owner * columns, 128), columns)
        ]

    sends = []
    for chunk in range(chunks):
        for step in range(1, lines):
            other = lax.rem(line + step, lines) * CORES + core
            copy = remote(
                x_ref.at[pl.ds(chunk * span, span)],
                place(me, chunk),
                send_sems.at[step, chunk],
                recv_sems.at[step, chunk],
                "tp",
                other,
            )
            copy.start()
            sends.append(copy)
    own = pltpu.make_async_copy(
        x_ref, out_ref.at[:, pl.ds(pl.multiple_of(me * columns, 128), columns)], local_sem
    )
    own.start()
    pairs = []
    for chunk in range(chunks):
        copy = remote(
            x_ref.at[pl.ds(chunk * span, span)],
            place(me, chunk),
            pair_send.at[0, chunk],
            pair_recv.at[0, chunk],
            "tp",
            pair,
        )
        copy.start()
        pairs.append(copy)
    for chunk in range(chunks):
        for step in range(1, lines):
            source = lax.rem(line + lines - step, lines) * CORES + core
            arrived = remote(
                place(source, chunk),
                place(source, chunk),
                send_sems.at[step, chunk],
                recv_sems.at[step, chunk],
                "tp",
                pair,
            )
            arrived.wait_recv()
            copy = remote(
                place(source, chunk),
                place(source, chunk),
                pair_send.at[step, chunk],
                pair_recv.at[step, chunk],
                "tp",
                pair,
            )
            copy.start()
            pairs.append(copy)
    own.wait()
    for copy in sends:
        copy.wait_send()
    for copy in pairs:
        copy.wait()


def head_mask(width, head):
    lanes = lax.broadcasted_iota(jnp.int32, (1, width), 1)
    return (lanes // HEAD) == head


def spread(columns, width):
    spreaded = columns[:, 0:1]
    for head in range(1, columns.shape[1]):
        lanes = lax.broadcasted_iota(jnp.int32, (1, width), 1)
        spreaded = jnp.where(lanes >= head * HEAD, columns[:, head : head + 1], spreaded)
    return jnp.broadcast_to(spreaded, (columns.shape[0], width))


def two_parts(floats):
    high = floats.astype(jnp.bfloat16)
    return high, (floats - high.astype(jnp.float32)).astype(jnp.bfloat16)


def dot(a, b, dims=((1,), (0,))):
    return lax.dot_general(a, b, (dims, ((), ())), preferred_element_type=jnp.float32)


def project_kernel(
    x_ref, gain_ref, cos_ref, sin_ref, wq, wk, wv, wmq, wmk, wmv, wi, wf, bias_ref, shift_ref,
    q_out, kv_out, mq_out, mk_out, mv_out, gate_out, gate_row_out, state_out,
    sq, sk, sv, smq, smk, smv, sems,
):
    copies = []
    for place, (source, target) in enumerate(
        ((wq, sq), (wk, sk), (wv, sv), (wmq, smq), (wmk, smk), (wmv, smv))
    ):
        copy = pltpu.make_async_copy(source, target, sems.at[place])
        copy.start()
        copies.append(copy)
    rows, features = x_ref.shape
    width = q_out.shape[1]
    heads = width // HEAD
    floats = x_ref[...].astype(jnp.float32)
    inverse = lax.rsqrt(
        jnp.sum(floats * floats, axis=1, keepdims=True) / features + EPSILON
    )
    scaled = (floats * gain_ref[...]).astype(jnp.bfloat16)
    gate = dot(scaled, wi[...]) * inverse
    pre = dot(scaled, wf[...]) * inverse + bias_ref[...]
    forget = jnp.minimum(pre, 0.0) - jnp.log1p(jnp.exp(-jnp.abs(pre))) + shift_ref[...]
    row_index = lax.broadcasted_iota(jnp.int32, (rows, rows), 0)
    column_index = lax.broadcasted_iota(jnp.int32, (rows, rows), 1)
    lower = (column_index <= row_index).astype(jnp.bfloat16)
    first, rest = two_parts(forget)
    second = (forget - first.astype(jnp.float32) - rest.astype(jnp.float32)).astype(jnp.bfloat16)
    cumulative = dot(lower, first) + (dot(lower, rest) + dot(lower, second))

    def product(place, scratch):
        copies[place].wait()
        return (dot(scaled, scratch[...]) * inverse).astype(jnp.bfloat16)

    lanes = lax.broadcasted_iota(jnp.int32, (1, width), 1)
    former = lax.rem(lanes, DD) < DD // 2

    def rotated(values):
        wide = values.astype(jnp.float32)
        partner = jnp.where(
            former, pltpu.roll(wide, width - DD // 2, 1), pltpu.roll(wide, DD // 2, 1)
        )
        return (wide * cos_ref[...] + partner * sin_ref[...]).astype(jnp.bfloat16)

    q_out[...] = rotated(product(0, sq))
    kv_out[:, :width] = rotated(product(1, sk))
    kv_out[:, width:] = product(2, sv)
    mq_out[...] = product(3, smq)
    memory_keys = product(4, smk)
    memory_values = product(5, smv)
    mk_out[...] = memory_keys
    mv_out[...] = memory_values

    end = cumulative[rows - 1 : rows, :]
    toward = end - cumulative + gate
    top = jnp.max(toward, axis=0, keepdims=True)
    weights = spread(jnp.exp(toward - top), width)
    keyed = memory_keys.astype(jnp.float32) * (HEAD**-0.5) * weights
    high, low = two_parts(keyed)
    whole = dot(high, memory_values, ((0,), (0,))) + dot(low, memory_values, ((0,), (0,)))
    memory = jnp.zeros((HEAD, width), jnp.float32)
    for head in range(heads):
        memory = jnp.where(
            head_mask(width, head), whole[head * HEAD : (head + 1) * HEAD, :], memory
        )
    state_out[:HEAD, :] = memory
    state_out[HEAD : HEAD + 1, :] = jnp.sum(keyed, axis=0, keepdims=True)
    state_out[HEAD + 1 : HEAD + 2, :] = spread(top, width)
    state_out[HEAD + 2 : HEAD + 3, :] = spread(end, width)
    state_out[HEAD + 3 :, :] = jnp.zeros((STATE_ROWS - HEAD - 3, width), jnp.float32)
    gate_out[...] = cumulative
    offsets = jnp.concatenate(
        [gate - cumulative, jnp.zeros((rows, 128 - heads), jnp.float32)], axis=1
    )
    gate_row_out[...] = offsets.T[:8, :]


def span_barrier(me, depth, across):
    z = me // across
    x = lax.rem(me, across)
    barrier = pltpu.get_barrier_semaphore()

    @pl.when(z > 0)
    def _():
        signal(barrier, "sp", me - across)

    @pl.when(z < depth - 1)
    def _():
        signal(barrier, "sp", me + across)

    for step in range(1, across):
        signal(barrier, "sp", z * across + lax.rem(x + step, across))
    beside = (z > 0).astype(jnp.int32) + (z < depth - 1).astype(jnp.int32)
    pl.semaphore_wait(barrier, across - 1 + beside)


def mixer_kernel(
    depth, across, q_ref, kv_ref, mq_ref, mk_ref, mv_ref, cumulative_ref, offset_ref, own_state_ref,
    lambda_ref, gain_ref, woa, wom, out_ref, attended_ref, memory_ref, soa, som,
    chosen_ref, top_ref, total_ref, sums_ref, kv_all, state_ref, sems,
    kv_send, kv_recv, st_send, st_recv,
):
    load_attention = pltpu.make_async_copy(woa, soa, sems.at[0])
    load_memory = pltpu.make_async_copy(wom, som, sems.at[1])
    load_attention.start()
    load_memory.start()
    me = lax.axis_index("sp")
    z = me // across
    x = lax.rem(me, across)
    span_barrier(me, depth, across)

    def transfers(back, target, slot, place, own):
        return [
            remote(
                mine if own else everything.at[slot],
                everything.at[slot],
                send.at[back, target],
                recv.at[slot],
                "sp",
                place,
            )
            for mine, everything, send, recv in (
                (own_state_ref, state_ref, st_send, st_recv),
                (kv_ref, kv_all, kv_send, kv_recv),
            )
        ]

    def arrived(slot):
        for copy in transfers(0, 0, slot, me, False):
            copy.wait_recv()

    def onward(back, act, own=False):
        slot = me - back * across
        for step in range(1, across):
            other = lax.rem(x + step, across)

            def sideways():
                for copy in transfers(back, step, slot, z * across + other, own):
                    act(copy)

            if own:
                pl.when(x < other)(sideways)
            else:
                sideways()

        @pl.when(z < depth - 1)
        def _():
            for copy in transfers(back, 0, slot, me + across, own):
                act(copy)

    onward(0, lambda copy: copy.start(), True)
    rows, width = q_ref.shape
    heads = width // HEAD
    row_index = lax.broadcasted_iota(jnp.int32, (rows, rows), 0)
    column_index = lax.broadcasted_iota(jnp.int32, (rows, rows), 1)
    lower = column_index <= row_index
    factor = (DD**-0.5) * LOG2E
    lanes = lax.broadcasted_iota(jnp.int32, (1, 128), 1)

    upper = row_index <= column_index
    for head in range(heads):
        group = slice(head // 2 * 128, head // 2 * 128 + 128)
        for half in range(2):
            chosen = (lanes // DD) == (head % 2) * 2 + half
            chosen_ref[head * 2 + half] = jnp.where(chosen, q_ref[:, group], 0)

    def block(source, diagonal):
        for head in range(heads):
            group = slice(head // 2 * 128, head // 2 * 128 + 128)
            value_group = slice(width + head // 2 * 128, width + head // 2 * 128 + 128)
            if head % 2 == 0:
                turned = source[:, value_group].T
            values = turned[(head % 2) * HEAD : (head % 2 + 1) * HEAD, :]
            for half in range(2):
                index = head * 2 + half
                at = slice(index, index + 1)
                rows_at = slice(index * HEAD, (index + 1) * HEAD)
                scores = dot(source[:, group], chosen_ref[index], ((1,), (1,)))
                if diagonal:
                    scores = jnp.where(upper, scores, NEGATIVE)
                top = jnp.max(scores, axis=0, keepdims=True)
                if not diagonal:
                    old_top = top_ref[at, :]
                    top = jnp.maximum(top, old_top)
                weights = jnp.exp2((scores - top) * factor)
                total = jnp.sum(weights, axis=0, keepdims=True)
                sums = dot(values, weights.astype(jnp.bfloat16))
                if not diagonal:
                    shrink = jnp.exp2((old_top - top) * factor)
                    total = total + total_ref[at, :] * shrink
                    sums = sums + sums_ref[rows_at, :] * shrink
                top_ref[at, :] = top
                total_ref[at, :] = total
                sums_ref[rows_at, :] = sums

    block(kv_ref, True)

    def beside(back):
        def one(step, unused):
            other = lax.rem(x + step, across)

            @pl.when((back > 0) | (other < x))
            def _():
                slot = (z - back) * across + other
                arrived(slot)
                block(kv_all.at[slot], False)

            return unused

        lax.fori_loop(1, across, one, 0)

    def earlier(back, unused):
        slot = me - back * across
        arrived(slot)
        onward(back, lambda copy: copy.start())
        beside(back - 1)
        block(kv_all.at[slot], False)
        return unused

    lax.fori_loop(1, z + 1, earlier, 0)
    beside(z)
    state = jnp.zeros((STATE_ROWS, width), jnp.float32)

    def advance(place, carried):
        body, stable = carried
        later = state_ref[place]
        later_top = later[HEAD + 1 : HEAD + 2, :]
        decay = later[HEAD + 2 : HEAD + 3, :]
        new = jnp.maximum(decay + stable, later_top)
        return jnp.exp(decay + stable - new) * body + jnp.exp(later_top - new) * later, new

    state, stable = lax.fori_loop(0, me, advance, (state, jnp.zeros((1, width), jnp.float32)))
    memory_in = state[:HEAD, :]
    normal_in = state[HEAD : HEAD + 1, :]
    blocks = jnp.concatenate(
        [jnp.where(head_mask(width, head), memory_in, 0.0) for head in range(heads)], axis=0
    )
    high, low = two_parts(blocks)
    memory_queries = mq_ref[...]
    carried_part = dot(memory_queries, high) + dot(memory_queries, low)
    weighted = memory_queries.astype(jnp.float32) * normal_in
    for group in range(width // 128):
        span = slice(group * 128, (group + 1) * 128)
        keys = mk_ref[:, span]
        values = mv_ref[:, span]
        group_queries = mq_ref[:, span]
        result = None
        for side in range(2):
            head = group * 2 + side
            chosen = (lanes // HEAD) == side
            column = cumulative_ref[:, head : head + 1]
            gaps = jnp.where(lower, column + offset_ref[head : head + 1, :], NEGATIVE)
            carried_log = column + stable[:, head * HEAD : head * HEAD + 1]
            row_top = jnp.maximum(carried_log, jnp.max(gaps, axis=1, keepdims=True))
            within = jnp.exp(gaps - row_top)
            outside = jnp.exp(carried_log - row_top)
            scores = dot(jnp.where(chosen, group_queries, 0), keys, ((1,), (1,)))
            scores = jnp.where(lower, within * (scores * (HEAD**-0.5)), 0.0)
            denominator = jnp.sum(scores, axis=1, keepdims=True) + outside * jnp.sum(
                jnp.where(chosen, weighted[:, span], 0.0), axis=1, keepdims=True
            )
            score_high, score_low = two_parts(scores)
            numerator = dot(score_high, values) + dot(score_low, values)
            numerator = numerator + outside * carried_part[:, span]
            quotient = numerator / jnp.maximum(jnp.abs(denominator), 1.0)
            result = quotient if result is None else jnp.where(chosen, quotient, result)
        memory_ref[:, span] = result.astype(jnp.bfloat16)

    for head in range(heads):
        first, second = (
            sums_ref[index * HEAD : (index + 1) * HEAD, :] / total_ref[index : index + 1, :]
            for index in (head * 2, head * 2 + 1)
        )
        difference = first - lambda_ref[:, head : head + 1] * second
        mean = jnp.mean(difference * difference, axis=0, keepdims=True)
        attended_ref[head * HEAD : (head + 1) * HEAD, :] = (
            difference * lax.rsqrt(mean + EPSILON) * gain_ref[...]
        ).astype(jnp.bfloat16)
    onward(0, lambda copy: copy.wait_send(), True)

    def finish(back, unused):
        onward(back, lambda copy: copy.wait_send())
        return unused

    lax.fori_loop(1, z + 1, finish, 0)
    load_attention.wait()
    load_memory.wait()
    out_ref[...] = (
        dot(attended_ref[...], soa[...], ((0,), (0,))) + dot(memory_ref[...], som[...])
    ).astype(jnp.bfloat16)


def scatter_kernel(size, chunks, part_ref, out_ref, pair_in, line_out, line_in, pair_send, pair_recv, line_send, line_recv):
    rows, columns = out_ref.shape
    lines = size // CORES
    me = lax.axis_index("tp")
    core = lax.rem(me, CORES)
    line = me // CORES
    pair = line * CORES + (1 - core)
    tp_barrier(me, lines)
    span = rows // chunks

    def columns_of(owner):
        return pl.ds(pl.multiple_of(owner * columns, 128), columns)

    def rows_of(chunk):
        return pl.ds(chunk * span, span)

    order = list(range(1, lines)) + [0]
    pairs = {}
    for chunk in range(chunks):
        for step in order:
            target = lax.rem(line + step, lines) * CORES + (1 - core)
            copy = remote(
                part_ref.at[rows_of(chunk), columns_of(target)],
                pair_in.at[step, rows_of(chunk)],
                pair_send.at[step, chunk],
                pair_recv.at[step, chunk],
                "tp",
                pair,
            )
            copy.start()
            pairs[step, chunk] = copy

    def pair_sum(step, chunk):
        pairs[step, chunk].wait_recv()
        mine = part_ref[rows_of(chunk), columns_of(lax.rem(line + step, lines) * CORES + core)]
        return mine.astype(jnp.float32) + pair_in[step, rows_of(chunk), :].astype(jnp.float32)

    sends = {}
    for chunk in range(chunks):
        for step in range(1, lines):
            line_out[step, rows_of(chunk), :] = pair_sum(step, chunk).astype(jnp.bfloat16)
            copy = remote(
                line_out.at[step, rows_of(chunk)],
                line_in.at[step, rows_of(chunk)],
                line_send.at[step, chunk],
                line_recv.at[step, chunk],
                "tp",
                lax.rem(line + step, lines) * CORES + core,
            )
            copy.start()
            sends[step, chunk] = copy
    for chunk in range(chunks):
        total = pair_sum(0, chunk)
        for step in range(1, lines):
            sends[step, chunk].wait_recv()
            total = total + line_in[step, rows_of(chunk), :].astype(jnp.float32)
        out_ref[rows_of(chunk), :] = total.astype(jnp.bfloat16)
    for copy in pairs.values():
        copy.wait_send()
    for copy in sends.values():
        copy.wait_send()


def per_device(tp_size, depth, across, inputs, norm_gain, query_weight, key_weight, value_weight,
               memory_query_weight, memory_key_weight, memory_value_weight, input_gate_weight,
               forget_gate_weight, forget_bias, decay_shift, lambdas, head_gain,
               out_weight_attention, out_weight_memory):
    rows, columns = inputs.shape
    features = norm_gain.shape[0]
    width = query_weight.shape[1]
    heads = width // HEAD
    lines = tp_size // CORES
    spans = depth * across
    chunks = 4
    dma = pltpu.SemaphoreType.DMA

    def params(**more):
        return pltpu.CompilerParams(vmem_limit_bytes=VMEM_LIMIT, **more)

    gathered = pl.pallas_call(
        functools.partial(gather_kernel, tp_size, chunks),
        out_shape=jax.ShapeDtypeStruct((rows, features), jnp.bfloat16),
        in_specs=[VMEM],
        out_specs=VMEM,
        scratch_shapes=[dma(()), dma((lines, chunks)), dma((lines, chunks)), dma((lines, chunks)), dma((lines, chunks))],
        compiler_params=params(collective_id=0, has_side_effects=True),
        name="gather_inputs",
    )(inputs)

    middle = DD // 2
    inverse = 1.0 / ROTARY_BASE ** (jnp.arange(middle, dtype=jnp.float32) / middle)
    positions = lax.axis_index("sp") * rows + jnp.arange(rows, dtype=jnp.int32)
    angles = positions.astype(jnp.float32)[:, None] * inverse[None, :]
    cosine = jnp.cos(angles)
    sine = jnp.sin(angles)
    cosine = jnp.tile(cosine, (1, width // middle))
    sine = jnp.tile(jnp.concatenate([-sine, sine], axis=1), (1, width // DD))

    hbm = pl.BlockSpec(memory_space=pl.ANY)
    half = jax.ShapeDtypeStruct((rows, width), jnp.bfloat16)
    queries, packed, memory_queries, memory_keys, memory_values, cumulative, offsets, state = pl.pallas_call(
        project_kernel,
        out_shape=[
            half,
            jax.ShapeDtypeStruct((rows, 2 * width), jnp.bfloat16),
            half,
            half,
            half,
            jax.ShapeDtypeStruct((rows, heads), jnp.float32),
            jax.ShapeDtypeStruct((8, rows), jnp.float32),
            jax.ShapeDtypeStruct((STATE_ROWS, width), jnp.float32),
        ],
        in_specs=[VMEM] * 4 + [hbm] * 6 + [VMEM] * 4,
        out_specs=[VMEM] * 8,
        scratch_shapes=[pltpu.VMEM((features, width), jnp.bfloat16)] * 6 + [dma((6,))],
        compiler_params=params(),
        name="project",
    )(
        gathered, norm_gain[None, :], cosine, sine, query_weight, key_weight, value_weight,
        memory_query_weight, memory_key_weight, memory_value_weight, input_gate_weight,
        forget_gate_weight, forget_bias[None, :], decay_shift,
    )

    partial_term = pl.pallas_call(
        functools.partial(mixer_kernel, depth, across),
        out_shape=jax.ShapeDtypeStruct((rows, features), jnp.bfloat16),
        in_specs=[VMEM] * 10 + [hbm] * 2,
        out_specs=VMEM,
        scratch_shapes=[
            pltpu.VMEM((width, rows), jnp.bfloat16),
            pltpu.VMEM((rows, width), jnp.bfloat16),
            pltpu.VMEM((width, features), jnp.bfloat16),
            pltpu.VMEM((width, features), jnp.bfloat16),
            pltpu.VMEM((2 * heads, rows, 128), jnp.bfloat16),
            pltpu.VMEM((2 * heads, rows), jnp.float32),
            pltpu.VMEM((2 * heads, rows), jnp.float32),
            pltpu.VMEM((2 * width, rows), jnp.float32),
            pltpu.VMEM((spans, rows, 2 * width), jnp.bfloat16),
            pltpu.VMEM((spans, STATE_ROWS, width), jnp.float32),
            dma((2,)), dma((depth, across)), dma((spans,)), dma((depth, across)), dma((spans,)),
        ],
        compiler_params=params(collective_id=1, has_side_effects=True),
        name="mixers",
    )(
        queries, packed, memory_queries, memory_keys, memory_values, cumulative, offsets,
        state, lambdas[None, :], head_gain[:, None], out_weight_attention,
        out_weight_memory,
    )

    return pl.pallas_call(
        functools.partial(scatter_kernel, tp_size, chunks),
        out_shape=jax.ShapeDtypeStruct((rows, columns), jnp.bfloat16),
        in_specs=[VMEM],
        out_specs=VMEM,
        scratch_shapes=[
            pltpu.VMEM((lines, rows, columns), jnp.bfloat16),
            pltpu.VMEM((lines, rows, columns), jnp.bfloat16),
            pltpu.VMEM((lines, rows, columns), jnp.bfloat16),
            dma((lines, chunks)), dma((lines, chunks)), dma((lines, chunks)), dma((lines, chunks)),
        ],
        compiler_params=params(collective_id=2, has_side_effects=True),
        name="scatter_output",
    )(partial_term)


def columns_across(mesh):
    spans = mesh.shape["sp"]
    try:
        places = {device.coords[0] for device in mesh.devices.flat}
        across = len(places)
    except AttributeError:
        across = 2
    return across if spans % across == 0 else 1


def solution(mesh):
    across = columns_across(mesh)
    in_specs = (
        P("sp", "tp"),
        P(),
        P(None, "tp"),
        P(None, "tp"),
        P(None, "tp"),
        P(None, "tp"),
        P(None, "tp"),
        P(None, "tp"),
        P(None, "tp"),
        P(None, "tp"),
        P("tp"),
        P("sp", "tp"),
        P("tp"),
        P(),
        P("tp", None),
        P("tp", None),
    )
    return jax.shard_map(
        functools.partial(
            per_device, mesh.shape["tp"], mesh.shape["sp"] // across, across
        ),
        mesh=mesh,
        in_specs=in_specs,
        out_specs=P("sp", "tp"),
        check_vma=False,
    )
```

```python
import functools

import jax
import jax.numpy as jnp
from jax import lax
from jax.experimental import pallas as pl
from jax.experimental.pallas import tpu as pltpu
from jax.sharding import PartitionSpec as P

HEAD = 64
DD = 32
EPSILON = 1e-06
ROTARY_BASE = 10000.0
NEGATIVE = -1e30
LOG2E = 1.4426950408889634
CORES = 2
STATE_ROWS = HEAD + 8
VMEM = pl.BlockSpec(memory_space=pltpu.VMEM)
MESH = pl.DeviceIdType.MESH
VMEM_LIMIT = 60 * 1024 * 1024


def signal(semaphore, axis, place):
    pl.semaphore_signal(semaphore, inc=1, device_id={axis: place}, device_id_type=MESH)


def remote(source, target, send_sem, recv_sem, axis, place):
    return pltpu.make_async_remote_copy(
        src_ref=source,
        dst_ref=target,
        send_sem=send_sem,
        recv_sem=recv_sem,
        device_id={axis: place},
        device_id_type=MESH,
    )


def tp_barrier(me, row_places):
    core = lax.rem(me, CORES)
    line = me // CORES
    barrier = pltpu.get_barrier_semaphore()
    signal(barrier, "tp", line * CORES + (1 - core))
    for step in range(1, row_places):
        signal(barrier, "tp", lax.rem(line + step, row_places) * CORES + core)
    pl.semaphore_wait(barrier, row_places)


def gather_kernel(size, chunks, x_ref, out_ref, local_sem, send_sems, recv_sems, pair_send, pair_recv):
    rows, columns = x_ref.shape
    lines = size // CORES
    me = lax.axis_index("tp")
    core = lax.rem(me, CORES)
    line = me // CORES
    pair = line * CORES + (1 - core)
    tp_barrier(me, lines)
    span = rows // chunks

    def place(owner, chunk):
        return out_ref.at[
            pl.ds(chunk * span, span), pl.ds(pl.multiple_of(owner * columns, 128), columns)
        ]

    sends = []
    for chunk in range(chunks):
        for step in range(1, lines):
            other = lax.rem(line + step, lines) * CORES + core
            copy = remote(
                x_ref.at[pl.ds(chunk * span, span)],
                place(me, chunk),
                send_sems.at[step, chunk],
                recv_sems.at[step, chunk],
                "tp",
                other,
            )
            copy.start()
            sends.append(copy)
    own = pltpu.make_async_copy(
        x_ref, out_ref.at[:, pl.ds(pl.multiple_of(me * columns, 128), columns)], local_sem
    )
    own.start()
    pairs = []
    for chunk in range(chunks):
        copy = remote(
            x_ref.at[pl.ds(chunk * span, span)],
            place(me, chunk),
            pair_send.at[0, chunk],
            pair_recv.at[0, chunk],
            "tp",
            pair,
        )
        copy.start()
        pairs.append(copy)
    for chunk in range(chunks):
        for step in range(1, lines):
            source = lax.rem(line + lines - step, lines) * CORES + core
            arrived = remote(
                place(source, chunk),
                place(source, chunk),
                send_sems.at[step, chunk],
                recv_sems.at[step, chunk],
                "tp",
                pair,
            )
            arrived.wait_recv()
            copy = remote(
                place(source, chunk),
                place(source, chunk),
                pair_send.at[step, chunk],
                pair_recv.at[step, chunk],
                "tp",
                pair,
            )
            copy.start()
            pairs.append(copy)
    own.wait()
    for copy in sends:
        copy.wait_send()
    for copy in pairs:
        copy.wait()


def head_mask(width, head):
    lanes = lax.broadcasted_iota(jnp.int32, (1, width), 1)
    return (lanes // HEAD) == head


def spread(columns, width):
    spreaded = columns[:, 0:1]
    for head in range(1, columns.shape[1]):
        lanes = lax.broadcasted_iota(jnp.int32, (1, width), 1)
        spreaded = jnp.where(lanes >= head * HEAD, columns[:, head : head + 1], spreaded)
    return jnp.broadcast_to(spreaded, (columns.shape[0], width))


def two_parts(floats):
    high = floats.astype(jnp.bfloat16)
    return high, (floats - high.astype(jnp.float32)).astype(jnp.bfloat16)


def dot(a, b, dims=((1,), (0,))):
    return lax.dot_general(a, b, (dims, ((), ())), preferred_element_type=jnp.float32)


def project_kernel(
    size, chunks, shard_ref, gain_ref, cos_ref, sin_ref, wq, wk, wv, wmq, wmk, wmv, wi, wf, bias_ref, shift_ref,
    q_out, kv_out, mq_out, mk_out, mv_out, gate_out, gate_row_out, state_out,
    sq, sk, sv, smq, smk, smv, sems, x_ref, local_sem, send_sems, recv_sems, pair_send, pair_recv,
):
    copies = []
    for place, (source, target) in enumerate(
        ((wq, sq), (wk, sk), (wv, sv), (wmq, smq), (wmk, smk), (wmv, smv))
    ):
        copy = pltpu.make_async_copy(source, target, sems.at[place])
        copy.start()
        copies.append(copy)
    gather_kernel(
        size, chunks, shard_ref, x_ref, local_sem, send_sems, recv_sems, pair_send, pair_recv
    )
    rows, features = x_ref.shape
    width = q_out.shape[1]
    heads = width // HEAD
    floats = x_ref[...].astype(jnp.float32)
    inverse = lax.rsqrt(
        jnp.sum(floats * floats, axis=1, keepdims=True) / features + EPSILON
    )
    scaled = (floats * gain_ref[...]).astype(jnp.bfloat16)
    gate = dot(scaled, wi[...], ((1,), (1,))) * inverse
    pre = dot(scaled, wf[...], ((1,), (1,))) * inverse + bias_ref[...]
    shift = shift_ref[...]
    shift = jnp.concatenate(
        [shift, jnp.zeros((128 - shift.shape[0], rows), jnp.float32)], axis=0
    ).T[:, : shift.shape[0]]
    forget = jnp.minimum(pre, 0.0) - jnp.log1p(jnp.exp(-jnp.abs(pre))) + shift
    row_index = lax.broadcasted_iota(jnp.int32, (rows, rows), 0)
    column_index = lax.broadcasted_iota(jnp.int32, (rows, rows), 1)
    lower = (column_index <= row_index).astype(jnp.bfloat16)
    first, rest = two_parts(forget)
    second = (forget - first.astype(jnp.float32) - rest.astype(jnp.float32)).astype(jnp.bfloat16)
    cumulative = dot(lower, first) + (dot(lower, rest) + dot(lower, second))

    def product(place, scratch):
        copies[place].wait()
        return (dot(scaled, scratch[...]) * inverse).astype(jnp.bfloat16)

    groups = width // 128
    cosine = jnp.concatenate([cos_ref[...]] * (128 * 2 // DD), axis=0).T
    sine = jnp.concatenate([-sin_ref[...], sin_ref[...]] * (128 // DD), axis=0).T
    cosine = jnp.concatenate([cosine] * groups, axis=1)
    sine = jnp.concatenate([sine] * groups, axis=1)
    lanes = lax.broadcasted_iota(jnp.int32, (1, width), 1)
    former = lax.rem(lanes, DD) < DD // 2

    def rotated(values):
        wide = values.astype(jnp.float32)
        partner = jnp.where(
            former, pltpu.roll(wide, width - DD // 2, 1), pltpu.roll(wide, DD // 2, 1)
        )
        return (wide * cosine + partner * sine).astype(jnp.bfloat16)

    q_out[...] = rotated(product(0, sq))
    kv_out[:, :width] = rotated(product(1, sk))
    kv_out[:, width:] = product(2, sv)
    mq_out[...] = product(3, smq)
    memory_keys = product(4, smk)
    memory_values = product(5, smv)
    mk_out[...] = memory_keys
    mv_out[...] = memory_values

    end = cumulative[rows - 1 : rows, :]
    toward = end - cumulative + gate
    top = jnp.max(toward, axis=0, keepdims=True)
    weights = spread(jnp.exp(toward - top), width)
    keyed = memory_keys.astype(jnp.float32) * (HEAD**-0.5) * weights
    high, low = two_parts(keyed)
    whole = dot(high, memory_values, ((0,), (0,))) + dot(low, memory_values, ((0,), (0,)))
    memory = jnp.zeros((HEAD, width), jnp.float32)
    for head in range(heads):
        memory = jnp.where(
            head_mask(width, head), whole[head * HEAD : (head + 1) * HEAD, :], memory
        )
    state_out[:HEAD, :] = memory
    state_out[HEAD : HEAD + 1, :] = jnp.sum(keyed, axis=0, keepdims=True)
    state_out[HEAD + 1 : HEAD + 2, :] = spread(top, width)
    state_out[HEAD + 2 : HEAD + 3, :] = spread(end, width)
    state_out[HEAD + 3 :, :] = jnp.zeros((STATE_ROWS - HEAD - 3, width), jnp.float32)
    gate_out[...] = cumulative
    offsets = jnp.concatenate(
        [gate - cumulative, jnp.zeros((rows, 128 - heads), jnp.float32)], axis=1
    )
    gate_row_out[...] = offsets.T[:8, :]


def span_barrier(me, depth, across):
    z = me // across
    x = lax.rem(me, across)
    barrier = pltpu.get_barrier_semaphore()

    @pl.when(z > 0)
    def _():
        signal(barrier, "sp", me - across)

    @pl.when(z < depth - 1)
    def _():
        signal(barrier, "sp", me + across)

    for step in range(1, across):
        signal(barrier, "sp", z * across + lax.rem(x + step, across))
    beside = (z > 0).astype(jnp.int32) + (z < depth - 1).astype(jnp.int32)
    pl.semaphore_wait(barrier, across - 1 + beside)


def mixer_kernel(
    depth, across, q_ref, kv_ref, mq_ref, mk_ref, mv_ref, cumulative_ref, offset_ref, own_state_ref,
    lambda_ref, gain_ref, woa, wom, out_ref, attended_ref, memory_ref, soa, som,
    chosen_ref, top_ref, total_ref, sums_ref, kv_all, state_ref, sems,
    kv_send, kv_recv, st_send, st_recv,
):
    load_attention = pltpu.make_async_copy(woa, soa, sems.at[0])
    load_memory = pltpu.make_async_copy(wom, som, sems.at[1])
    load_attention.start()
    load_memory.start()
    me = lax.axis_index("sp")
    z = me // across
    x = lax.rem(me, across)
    span_barrier(me, depth, across)

    def transfers(back, target, slot, place, own):
        return [
            remote(
                mine if own else everything.at[slot],
                everything.at[slot],
                send.at[back, target],
                recv.at[slot],
                "sp",
                place,
            )
            for mine, everything, send, recv in (
                (own_state_ref, state_ref, st_send, st_recv),
                (kv_ref, kv_all, kv_send, kv_recv),
            )
        ]

    def arrived(slot):
        for copy in transfers(0, 0, slot, me, False):
            copy.wait_recv()

    def onward(back, act, own=False):
        slot = me - back * across
        for step in range(1, across):
            other = lax.rem(x + step, across)

            def sideways():
                for copy in transfers(back, step, slot, z * across + other, own):
                    act(copy)

            if own:
                pl.when(x < other)(sideways)
            else:
                sideways()

        @pl.when(z < depth - 1)
        def _():
            for copy in transfers(back, 0, slot, me + across, own):
                act(copy)

    onward(0, lambda copy: copy.start(), True)
    rows, width = q_ref.shape
    heads = width // HEAD
    row_index = lax.broadcasted_iota(jnp.int32, (rows, rows), 0)
    column_index = lax.broadcasted_iota(jnp.int32, (rows, rows), 1)
    lower = column_index <= row_index
    factor = (DD**-0.5) * LOG2E
    lanes = lax.broadcasted_iota(jnp.int32, (1, 128), 1)

    upper = row_index <= column_index
    for head in range(heads):
        group = slice(head // 2 * 128, head // 2 * 128 + 128)
        for half in range(2):
            chosen = (lanes // DD) == (head % 2) * 2 + half
            chosen_ref[head * 2 + half] = jnp.where(chosen, q_ref[:, group], 0)

    def block(source, diagonal):
        for head in range(heads):
            group = slice(head // 2 * 128, head // 2 * 128 + 128)
            value_group = slice(width + head // 2 * 128, width + head // 2 * 128 + 128)
            if head % 2 == 0:
                turned = source[:, value_group].T
            values = turned[(head % 2) * HEAD : (head % 2 + 1) * HEAD, :]
            for half in range(2):
                index = head * 2 + half
                at = slice(index, index + 1)
                rows_at = slice(index * HEAD, (index + 1) * HEAD)
                scores = dot(source[:, group], chosen_ref[index], ((1,), (1,)))
                if diagonal:
                    scores = jnp.where(upper, scores, NEGATIVE)
                top = jnp.max(scores, axis=0, keepdims=True)
                if not diagonal:
                    old_top = top_ref[at, :]
                    top = jnp.maximum(top, old_top)
                weights = jnp.exp2((scores - top) * factor)
                total = jnp.sum(weights, axis=0, keepdims=True)
                sums = dot(values, weights.astype(jnp.bfloat16))
                if not diagonal:
                    shrink = jnp.exp2((old_top - top) * factor)
                    total = total + total_ref[at, :] * shrink
                    sums = sums + sums_ref[rows_at, :] * shrink
                top_ref[at, :] = top
                total_ref[at, :] = total
                sums_ref[rows_at, :] = sums

    block(kv_ref, True)

    def beside(back):
        def one(step, unused):
            other = lax.rem(x + step, across)

            @pl.when((back > 0) | (other < x))
            def _():
                slot = (z - back) * across + other
                arrived(slot)
                block(kv_all.at[slot], False)

            return unused

        lax.fori_loop(1, across, one, 0)

    def earlier(back, unused):
        slot = me - back * across
        arrived(slot)
        onward(back, lambda copy: copy.start())
        beside(back - 1)
        block(kv_all.at[slot], False)
        return unused

    lax.fori_loop(1, z + 1, earlier, 0)
    beside(z)
    state = jnp.zeros((STATE_ROWS, width), jnp.float32)

    def advance(place, carried):
        body, stable = carried
        later = state_ref[place]
        later_top = later[HEAD + 1 : HEAD + 2, :]
        decay = later[HEAD + 2 : HEAD + 3, :]
        new = jnp.maximum(decay + stable, later_top)
        return jnp.exp(decay + stable - new) * body + jnp.exp(later_top - new) * later, new

    state, stable = lax.fori_loop(0, me, advance, (state, jnp.zeros((1, width), jnp.float32)))
    memory_in = state[:HEAD, :]
    normal_in = state[HEAD : HEAD + 1, :]
    blocks = jnp.concatenate(
        [jnp.where(head_mask(width, head), memory_in, 0.0) for head in range(heads)], axis=0
    )
    high, low = two_parts(blocks)
    memory_queries = mq_ref[...]
    carried_part = dot(memory_queries, high) + dot(memory_queries, low)
    weighted = memory_queries.astype(jnp.float32) * normal_in
    for group in range(width // 128):
        span = slice(group * 128, (group + 1) * 128)
        keys = mk_ref[:, span]
        values = mv_ref[:, span]
        group_queries = mq_ref[:, span]
        result = None
        for side in range(2):
            head = group * 2 + side
            chosen = (lanes // HEAD) == side
            column = cumulative_ref[:, head : head + 1]
            gaps = jnp.where(lower, column + offset_ref[head : head + 1, :], NEGATIVE)
            carried_log = column + stable[:, head * HEAD : head * HEAD + 1]
            row_top = jnp.maximum(carried_log, jnp.max(gaps, axis=1, keepdims=True))
            within = jnp.exp(gaps - row_top)
            outside = jnp.exp(carried_log - row_top)
            scores = dot(jnp.where(chosen, group_queries, 0), keys, ((1,), (1,)))
            scores = jnp.where(lower, within * (scores * (HEAD**-0.5)), 0.0)
            denominator = jnp.sum(scores, axis=1, keepdims=True) + outside * jnp.sum(
                jnp.where(chosen, weighted[:, span], 0.0), axis=1, keepdims=True
            )
            score_high, score_low = two_parts(scores)
            numerator = dot(score_high, values) + dot(score_low, values)
            numerator = numerator + outside * carried_part[:, span]
            quotient = numerator / jnp.maximum(jnp.abs(denominator), 1.0)
            result = quotient if result is None else jnp.where(chosen, quotient, result)
        memory_ref[:, span] = result.astype(jnp.bfloat16)

    eye = lax.broadcasted_iota(jnp.int32, (HEAD, HEAD), 0) == lax.broadcasted_iota(
        jnp.int32, (HEAD, HEAD), 1
    )
    gain = jnp.sum(jnp.where(eye, gain_ref[...], 0.0), axis=1, keepdims=True)
    for head in range(heads):
        first, second = (
            sums_ref[index * HEAD : (index + 1) * HEAD, :] / total_ref[index : index + 1, :]
            for index in (head * 2, head * 2 + 1)
        )
        difference = first - lambda_ref[:, head : head + 1] * second
        mean = jnp.mean(difference * difference, axis=0, keepdims=True)
        attended_ref[head * HEAD : (head + 1) * HEAD, :] = (
            difference * lax.rsqrt(mean + EPSILON) * gain
        ).astype(jnp.bfloat16)
    onward(0, lambda copy: copy.wait_send(), True)

    def finish(back, unused):
        onward(back, lambda copy: copy.wait_send())
        return unused

    lax.fori_loop(1, z + 1, finish, 0)
    load_attention.wait()
    load_memory.wait()
    out_ref[...] = (
        dot(attended_ref[...], soa[...], ((0,), (0,))) + dot(memory_ref[...], som[...])
    ).astype(jnp.bfloat16)


def scatter_kernel(size, chunks, part_ref, out_ref, pair_in, line_out, line_in, pair_send, pair_recv, line_send, line_recv):
    rows, columns = out_ref.shape
    lines = size // CORES
    me = lax.axis_index("tp")
    core = lax.rem(me, CORES)
    line = me // CORES
    pair = line * CORES + (1 - core)
    tp_barrier(me, lines)
    span = rows // chunks

    def columns_of(owner):
        return pl.ds(pl.multiple_of(owner * columns, 128), columns)

    def rows_of(chunk):
        return pl.ds(chunk * span, span)

    order = list(range(1, lines)) + [0]
    pairs = {}
    for chunk in range(chunks):
        for step in order:
            target = lax.rem(line + step, lines) * CORES + (1 - core)
            copy = remote(
                part_ref.at[rows_of(chunk), columns_of(target)],
                pair_in.at[step, rows_of(chunk)],
                pair_send.at[step, chunk],
                pair_recv.at[step, chunk],
                "tp",
                pair,
            )
            copy.start()
            pairs[step, chunk] = copy

    def pair_sum(step, chunk):
        pairs[step, chunk].wait_recv()
        mine = part_ref[rows_of(chunk), columns_of(lax.rem(line + step, lines) * CORES + core)]
        return mine.astype(jnp.float32) + pair_in[step, rows_of(chunk), :].astype(jnp.float32)

    sends = {}
    for chunk in range(chunks):
        for step in range(1, lines):
            line_out[step, rows_of(chunk), :] = pair_sum(step, chunk).astype(jnp.bfloat16)
            copy = remote(
                line_out.at[step, rows_of(chunk)],
                line_in.at[step, rows_of(chunk)],
                line_send.at[step, chunk],
                line_recv.at[step, chunk],
                "tp",
                lax.rem(line + step, lines) * CORES + core,
            )
            copy.start()
            sends[step, chunk] = copy
    for chunk in range(chunks):
        total = pair_sum(0, chunk)
        for step in range(1, lines):
            sends[step, chunk].wait_recv()
            total = total + line_in[step, rows_of(chunk), :].astype(jnp.float32)
        out_ref[rows_of(chunk), :] = total.astype(jnp.bfloat16)
    for copy in pairs.values():
        copy.wait_send()
    for copy in sends.values():
        copy.wait_send()


def per_device(tp_size, depth, across, inputs, norm_gain, query_weight, key_weight, value_weight,
               memory_query_weight, memory_key_weight, memory_value_weight, input_gate_weight,
               forget_gate_weight, forget_bias, decay_shift, lambdas, head_gain,
               out_weight_attention, out_weight_memory):
    rows, columns = inputs.shape
    features = norm_gain.shape[0]
    width = query_weight.shape[1]
    heads = width // HEAD
    lines = tp_size // CORES
    spans = depth * across
    chunks = 4
    dma = pltpu.SemaphoreType.DMA

    def params(**more):
        return pltpu.CompilerParams(vmem_limit_bytes=VMEM_LIMIT, **more)

    middle = DD // 2
    inverse = 1.0 / ROTARY_BASE ** (jnp.arange(middle, dtype=jnp.float32) / middle)
    positions = lax.axis_index("sp") * rows + jnp.arange(rows, dtype=jnp.int32)
    angles = inverse[:, None] * positions.astype(jnp.float32)[None, :]
    cosine = jnp.cos(angles)
    sine = jnp.sin(angles)

    hbm = pl.BlockSpec(memory_space=pl.ANY)
    half = jax.ShapeDtypeStruct((rows, width), jnp.bfloat16)
    queries, packed, memory_queries, memory_keys, memory_values, cumulative, offsets, state = pl.pallas_call(
        functools.partial(project_kernel, tp_size, chunks),
        out_shape=[
            half,
            jax.ShapeDtypeStruct((rows, 2 * width), jnp.bfloat16),
            half,
            half,
            half,
            jax.ShapeDtypeStruct((rows, heads), jnp.float32),
            jax.ShapeDtypeStruct((8, rows), jnp.float32),
            jax.ShapeDtypeStruct((STATE_ROWS, width), jnp.float32),
        ],
        in_specs=[VMEM] * 4 + [hbm] * 6 + [VMEM] * 4,
        out_specs=[VMEM] * 8,
        scratch_shapes=[pltpu.VMEM((features, width), jnp.bfloat16)] * 6
        + [dma((6,)), pltpu.VMEM((rows, features), jnp.bfloat16), dma(())]
        + [dma((lines, chunks))] * 4,
        compiler_params=params(collective_id=0, has_side_effects=True),
        name="project",
    )(
        inputs, norm_gain[None, :], cosine, sine, query_weight, key_weight, value_weight,
        memory_query_weight, memory_key_weight, memory_value_weight, input_gate_weight.T,
        forget_gate_weight.T, forget_bias[None, :], decay_shift.T,
    )

    partial_term = pl.pallas_call(
        functools.partial(mixer_kernel, depth, across),
        out_shape=jax.ShapeDtypeStruct((rows, features), jnp.bfloat16),
        in_specs=[VMEM] * 10 + [hbm] * 2,
        out_specs=VMEM,
        scratch_shapes=[
            pltpu.VMEM((width, rows), jnp.bfloat16),
            pltpu.VMEM((rows, width), jnp.bfloat16),
            pltpu.VMEM((width, features), jnp.bfloat16),
            pltpu.VMEM((width, features), jnp.bfloat16),
            pltpu.VMEM((2 * heads, rows, 128), jnp.bfloat16),
            pltpu.VMEM((2 * heads, rows), jnp.float32),
            pltpu.VMEM((2 * heads, rows), jnp.float32),
            pltpu.VMEM((2 * width, rows), jnp.float32),
            pltpu.VMEM((spans, rows, 2 * width), jnp.bfloat16),
            pltpu.VMEM((spans, STATE_ROWS, width), jnp.float32),
            dma((2,)), dma((depth, across)), dma((spans,)), dma((depth, across)), dma((spans,)),
        ],
        compiler_params=params(collective_id=1, has_side_effects=True),
        name="mixers",
    )(
        queries, packed, memory_queries, memory_keys, memory_values, cumulative, offsets,
        state, lambdas[None, :], head_gain[None, :], out_weight_attention,
        out_weight_memory,
    )

    return pl.pallas_call(
        functools.partial(scatter_kernel, tp_size, chunks),
        out_shape=jax.ShapeDtypeStruct((rows, columns), jnp.bfloat16),
        in_specs=[VMEM],
        out_specs=VMEM,
        scratch_shapes=[
            pltpu.VMEM((lines, rows, columns), jnp.bfloat16),
            pltpu.VMEM((lines, rows, columns), jnp.bfloat16),
            pltpu.VMEM((lines, rows, columns), jnp.bfloat16),
            dma((lines, chunks)), dma((lines, chunks)), dma((lines, chunks)), dma((lines, chunks)),
        ],
        compiler_params=params(collective_id=2, has_side_effects=True),
        name="scatter_output",
    )(partial_term)


def columns_across(mesh):
    spans = mesh.shape["sp"]
    try:
        places = {device.coords[0] for device in mesh.devices.flat}
        across = len(places)
    except AttributeError:
        across = 2
    return across if spans % across == 0 else 1


def solution(mesh):
    across = columns_across(mesh)
    in_specs = (
        P("sp", "tp"),
        P(),
        P(None, "tp"),
        P(None, "tp"),
        P(None, "tp"),
        P(None, "tp"),
        P(None, "tp"),
        P(None, "tp"),
        P(None, "tp"),
        P(None, "tp"),
        P("tp"),
        P("sp", "tp"),
        P("tp"),
        P(),
        P("tp", None),
        P("tp", None),
    )
    return jax.shard_map(
        functools.partial(
            per_device, mesh.shape["tp"], mesh.shape["sp"] // across, across
        ),
        mesh=mesh,
        in_specs=in_specs,
        out_specs=P("sp", "tp"),
        check_vma=False,
    )
```
